256 devices in a mesh: grp: 2 (over y), ep: 32 (over z, core), tp: 4 (over x).
Axes of the slice: x: 4, y: 2, z: 16, core: 2. Of those that a mesh axis runs over, the one named last changes fastest.
The devices are a block of a 4x16x16 slice.
Arguments:
- queries: bfloat16 [8192, 2048], P(('grp', 'ep'), 'tp'), parts along dimension 0, may hold values from -6 to 6
- keys: bfloat16 [8192, 2048], P(('grp', 'ep'), 'tp'), parts along dimension 0, may hold values from -6 to 6
- values: bfloat16 [8192, 2048], P(('grp', 'ep'), 'tp'), parts along dimension 0, may hold values from -6 to 6
- stop_bias: bfloat16 [8192, 32], P(('grp', 'ep'), 'tp'), parts along dimension 0, may hold values from -20 to 0
- out_weight: bfloat16 [2048, 2048], P('tp'), may hold values from -0.125 to 0.125
- mix_gain: float32 [2048], replicated, may hold values from 0.1 to 1.9
- moe_input: bfloat16 [32768, 2048], P(('grp', 'ep', 'tp')), parts along dimension 0, may hold values from -6 to 6
- ffn_gain: float32 [2048], replicated, may hold values from 0.1 to 1.9
- expert_ids: int32 [32768, 2], P(('grp', 'ep', 'tp')), parts along dimension 0, may hold values from 0 to 31, all different within a row; in each aligned block of 128 rows (0 to 127, 128 to 255, ...) at most 12 rows name the same one
- expert_scores: float32 [32768, 2], P(('grp', 'ep', 'tp')), parts along dimension 0, may hold values from 0.05 to 1
- gate_weight: bfloat16 [32, 2048, 1024], P('ep', None, 'tp'), may hold values from -0.125 to 0.125
- up_weight: bfloat16 [32, 2048, 1024], P('ep', None, 'tp'), may hold values from -0.125 to 0.125
- down_weight: bfloat16 [32, 1024, 2048], P('ep', 'tp'), may hold values from -0.1875 to 0.1875
Outputs:
- mixed: bfloat16 [8192, 2048], P(('grp', 'ep', 'tp')), parts along dimension 0
- experts_mixed: bfloat16 [32768, 2048], P(('grp', 'ep', 'tp')), parts along dimension 0
The draws below stay inside these ranges and needn't reach their ends.
There are 2 independent parts, one for each index of `grp`. The reference program is written for one: setup_inputs(seed, part) draws one part's arguments, and reference() takes and returns one part's arrays. A program takes and returns all parts, laid end to end along the dimension named above; an argument that names none is the same for every part. Nothing has to cross between parts.
Inputs may be any that keep to these rules, and one draw needn't show every extreme that they name: `expert_ids`: each token names 2 different experts. Among the 128 tokens of one device, no expert is named by more than 12 tokens, and in some device's tokens some expert is named by exactly 12.
All inputs are finite; a program needn't handle non-finite values.
Results may differ from the reference program's by a relative error of at most 0.012.
Values may be sent and summed in bfloat16 or wider, within the bound.
A program may use at most 128 MiB of HBM per device.

```python
import math
import jax
import jax.numpy as jnp
import numpy as np
from jax import lax

D = 2048
HEADS = 32
HEAD = 64
FF = 1024
TOP_K = 2
SEQ_DEV = 128
TOK_DEV = 128
CONTEXT_LENGTH = 4096
TOKENS = 16384
EXPERTS = 32
CAP = 12
N_EP = 32
N_TP = 4


def draw_stop_bias(key, part):
    streams = jax.random.split(key, 7)
    fast = jax.random.uniform(streams[0], (HEADS,)) < 0.5
    slow_rate = jax.random.uniform(streams[1], (HEADS,), minval=0.1, maxval=0.4) / CONTEXT_LENGTH
    fast_rate = jax.random.uniform(streams[2], (HEADS,), minval=1.0 / 150.0, maxval=1.0 / 60.0)
    starting_level = jnp.log(jnp.where(fast, fast_rate, slow_rate))
    displacement_delta = jax.random.uniform(streams[3], (CONTEXT_LENGTH // SEQ_DEV, 1), minval=-0.7, maxval=0.7)
    displacement_delta = jnp.repeat(displacement_delta, SEQ_DEV, axis=0)
    approximate_guess = jax.random.uniform(streams[4], (CONTEXT_LENGTH, HEADS), minval=-2.0, maxval=2.0)
    location_number = jax.random.randint(streams[5], (4,), 0, CONTEXT_LENGTH)
    spike_height = jnp.any(jnp.arange(CONTEXT_LENGTH)[:, None] == location_number[None, :], axis=1)
    intensity_multiplier = jax.random.uniform(streams[6], (CONTEXT_LENGTH, HEADS), minval=0.25, maxval=0.4)
    closing_answer = jnp.where(spike_height[:, None], jnp.log(intensity_multiplier / (1.0 - intensity_multiplier)), starting_level[None, :] + displacement_delta + approximate_guess)
    return closing_answer.astype(jnp.bfloat16)


def level_of(key, extent, cuts, low, largest):
    def one(position, blocks):
        heights = jax.random.uniform(jax.random.fold_in(jax.random.fold_in(key, 6), position), (blocks,), jnp.float32, low / len(cuts), largest / len(cuts))
        return jnp.repeat(jnp.exp(heights), extent[position] // blocks).reshape((-1,) + (1,) * (len(extent) - position - 1))

    loudness = one(*cuts[0])
    for cut in cuts[1:]:
        loudness = loudness * one(*cut)
    return loudness


def routed_block(stream_key, own, number, rows, amount, top, limit, slope):
    sequence = jax.random.permutation(stream_key, amount)
    heavy_load, usual = shares(amount, rows * top, limit, slope, True), shares(amount, rows * top, limit, slope, False)
    places = jnp.arange(amount)

    def named(tallies, turn):
        used = int((tallies > 0).sum())
        fixed = max(1, used // 4)
        shifted = fixed + (places - fixed + turn * (used - fixed)) % max(1, amount - fixed)
        return jnp.zeros((amount,), jnp.int32).at[sequence[jnp.where(places < fixed, places, shifted)]].set(jnp.asarray(tallies, jnp.int32))

    tallies = jnp.where(number % 4 == 0, named(heavy_load, number // 4), named(usual, number - number // 4 - 1))
    mixed = jax.random.permutation(jax.random.fold_in(own, 3), amount)
    giver, sink = mixed[0:amount // 2 * 2:2], mixed[1:amount // 2 * 2:2]
    margin = jnp.minimum(tallies[giver] - 1, limit - tallies[sink]) // 2
    margin = jnp.where((giver == sequence[0]) | (sink == sequence[0]) | (tallies[sink] == 0), 0, jnp.maximum(margin, 0))
    shifted = jax.random.randint(jax.random.fold_in(own, 4), (amount // 2,), 0, 1 << 20) % (margin + 1)
    tallies = tallies.at[giver].add(-shifted).at[sink].add(shifted)
    members = jnp.searchsorted(jnp.cumsum(tallies), jnp.arange(rows * top), side="right").astype(jnp.int32)
    table = members.reshape(top, rows).T
    table = table[jax.random.permutation(jax.random.fold_in(own, 1), rows)]
    turn = jax.random.randint(jax.random.fold_in(own, 2), (rows, 1), 0, top)
    return jnp.take_along_axis(table, (jnp.arange(top)[None, :] + turn) % top, axis=1)


def shares(number_of, total, bound, skew, full):
    loads = [(1 << 20) // math.isqrt(standing ** skew) + 1 for standing in range(1, number_of + 1)]
    largest = bound if full else min(bound, max(-(-total // number_of), total * loads[0] // sum(loads)))
    least = 1 if total - largest >= number_of - 1 else 0
    counts, spare = [largest] + [least] * (number_of - 1), total - largest - least * (number_of - 1)
    while spare > 0:
        candidates = [i for i in range(1, number_of) if counts[i] < largest] or [i for i in range(1, number_of) if counts[i] < bound]
        mass, remaining = sum([loads[i] for i in candidates]), spare
        for i in candidates:
            addition = min(bound - counts[i], max(1, remaining * loads[i] // mass), spare)
            counts[i] = counts[i] + addition
            spare = spare - addition
    return np.array(counts)


def scatter_about(own_key, shape, scale, bound, cuts=(), held_as=jnp.bfloat16):
    values = jax.random.normal(own_key, shape, jnp.float32) * scale
    if len(cuts) > 0:
        values = level_of(own_key, shape, cuts, -0.22, 0.18) * values
    return jnp.clip(values, min=-bound, max=bound).astype(held_as)


def setup_inputs(seed: int = 0, part: int = 0) -> dict:
    key_of = jax.random.split(jax.random.key(seed), 14)
    own_keys = jax.random.split(jax.random.fold_in(key_of[13], part), 14)
    queries = scatter_about(own_keys[0], (CONTEXT_LENGTH, HEADS * HEAD), 1.0, 6.0, ((0, 32), (1, 4)))
    keys = scatter_about(own_keys[1], (CONTEXT_LENGTH, HEADS * HEAD), 1.0, 6.0, ((0, 32), (1, 4)))
    values = scatter_about(own_keys[2], (CONTEXT_LENGTH, HEADS * HEAD), 1.0, 6.0, ((0, 32), (1, 4)))
    stop_bias = draw_stop_bias(jax.random.fold_in(jax.random.fold_in(key_of[13], part), 71), part)
    out_weight = scatter_about(key_of[4], (HEADS * HEAD, D), (HEADS * HEAD) ** -0.5, 0.125, ((0, 4),))
    mix_gain = jnp.clip(1.0 + 0.18 * jax.random.normal(key_of[5], (D,), jnp.float32), 0.1, 1.9)
    moe_input = scatter_about(own_keys[6], (TOKENS, D), 1.0, 6.0, ((0, 128),))
    ffn_gain = jnp.clip(1.0 + 0.18 * jax.random.normal(key_of[7], (D,), jnp.float32), 0.1, 1.9)
    expert_ids_keys = jax.random.split(jax.random.fold_in(own_keys[8], 1), TOKENS // TOK_DEV)
    expert_ids_turns = jax.random.permutation(jax.random.fold_in(own_keys[8], 3), TOKENS // TOK_DEV)
    expert_ids = jax.vmap(lambda own, number: routed_block(jax.random.fold_in(own_keys[8], 2), own, number, TOK_DEV, EXPERTS, TOP_K, CAP, 2))(expert_ids_keys, expert_ids_turns).reshape((TOKENS, TOP_K))
    expert_scores = jnp.clip(jnp.exp(math.log(1.0) - 2.9957323 * jax.random.uniform(own_keys[9], (TOKENS, TOP_K), jnp.float32) ** level_of(own_keys[9], (TOKENS, TOP_K), ((0, 128),), -0.2, 0.2)), 0.05, 1.0)
    gate_weight = scatter_about(key_of[10], (EXPERTS, D, FF), D ** -0.5, 0.125, ((0, 32), (2, 4)))
    up_weight = scatter_about(key_of[11], (EXPERTS, D, FF), D ** -0.5, 0.125, ((0, 32), (2, 4)))
    down_weight = scatter_about(key_of[12], (EXPERTS, FF, D), FF ** -0.5, 0.1875, ((0, 32), (1, 4)))
    return dict(queries=queries, keys=keys, values=values, stop_bias=stop_bias, out_weight=out_weight, mix_gain=mix_gain, moe_input=moe_input, ffn_gain=ffn_gain, expert_ids=expert_ids, expert_scores=expert_scores, gate_weight=gate_weight, up_weight=up_weight, down_weight=down_weight)


def norm_rows(values, gain):
    values = values.astype(jnp.float32)
    scale = lax.rsqrt(lax.optimization_barrier(jnp.mean(values * values, axis=-1, keepdims=True)) + 1e-06)
    return values * scale * gain

def settle(term):
    return lax.optimization_barrier(term.astype(jnp.bfloat16)).astype(jnp.float32)

def stick_head(inputs):
    query, key, value, bias = inputs
    length = query.shape[0]
    count = length // SEQ_DEV
    scores = jnp.dot(query, key.T, preferred_element_type=jnp.float32) * HEAD ** (-0.5)
    scores = scores + bias.astype(jnp.float32)[None, :]
    place = jnp.arange(length)
    past = place[None, :] < place[:, None]
    rest = jnp.where(past, jax.nn.log_sigmoid(-scores), 0.0)
    rest_blocks = rest.reshape(length, count, SEQ_DEV)
    later = lax.cumsum(rest_blocks, axis=2, reverse=True)
    within = (later - rest_blocks).reshape(length, length)
    totals = later[:, :, 0]
    local = jnp.where(past, jnp.exp(jax.nn.log_sigmoid(scores) + within), 0.0).astype(jnp.bfloat16)
    parts = jnp.einsum('tbs,bsd->tbd', local.reshape(length, count, SEQ_DEV).astype(jnp.float32), value.reshape(count, SEQ_DEV, HEAD).astype(jnp.float32), precision=lax.Precision.HIGHEST)
    carried = lax.cumsum(totals, axis=1, reverse=True) - totals
    return lax.optimization_barrier(jnp.sum(jnp.exp(carried)[:, :, None] * parts, axis=1))

def reference(queries, keys, values, stop_bias, out_weight, mix_gain, moe_input, ffn_gain, expert_ids, expert_scores, gate_weight, up_weight, down_weight):
    length = queries.shape[0]

    def by_head(array):
        return array.reshape(length, HEADS, HEAD).transpose(1, 0, 2)
    attended = lax.map(stick_head, (by_head(queries), by_head(keys), by_head(values), stop_bias.T))
    attended = attended.transpose(1, 0, 2).reshape(length, HEADS * HEAD).astype(jnp.bfloat16)
    group = HEADS * HEAD // N_TP
    projected = jnp.zeros((length, D), jnp.float32)
    for quarter in range(N_TP):
        term = jnp.dot(attended[:, quarter * group:(quarter + 1) * group], out_weight[quarter * group:(quarter + 1) * group], preferred_element_type=jnp.float32)
        projected = projected + settle(term)
    mixed = norm_rows(projected, mix_gain).astype(jnp.bfloat16)
    normed = norm_rows(moe_input, ffn_gain).astype(jnp.bfloat16)
    weights = expert_scores / lax.optimization_barrier(jnp.sum(expert_scores, axis=1, keepdims=True))
    load = N_EP * N_TP * CAP
    share = FF // N_TP

    def one_expert(total, expert):
        named = expert_ids == expert
        present = jnp.any(named, axis=1)
        weight = lax.optimization_barrier(jnp.sum(jnp.where(named, weights, 0.0), axis=1))
        chosen = jnp.nonzero(present, size=load, fill_value=0)[0].astype(jnp.int32)
        valid = jnp.arange(load) < jnp.sum(present.astype(jnp.int32))
        rows = normed[chosen]
        gate = jnp.dot(rows, gate_weight[expert], preferred_element_type=jnp.float32)
        upward = jnp.dot(rows, up_weight[expert], preferred_element_type=jnp.float32)
        hidden = (jax.nn.silu(gate) * upward).astype(jnp.bfloat16)
        lowering = down_weight[expert]
        summed = jnp.zeros((load, D), jnp.float32)
        for quarter in range(N_TP):
            term = jnp.dot(hidden[:, quarter * share:(quarter + 1) * share], lowering[quarter * share:(quarter + 1) * share], preferred_element_type=jnp.float32)
            summed = summed + settle(term)
        output = settle(summed)
        contribution = jnp.where(valid[:, None], weight[chosen][:, None] * output, 0.0)
        return (total.at[chosen].add(contribution), None)
    total, _ = lax.scan(one_expert, jnp.zeros((TOKENS, D), jnp.float32), jnp.arange(EXPERTS, dtype=jnp.int32))
    return (mixed, total.astype(jnp.bfloat16))
```

```python
import functools

import jax
import jax.numpy as jnp
from jax import lax
from jax.experimental import pallas as pl
from jax.experimental.pallas import tpu as pltpu
from jax.sharding import PartitionSpec as P

MESH = pl.DeviceIdType.MESH
BF16 = jnp.bfloat16
F32 = jnp.float32
GRP_EP = ("grp", "ep")
GRP_EP_TP = ("grp", "ep", "tp")
ROWS = 8


def dot(a, b):
    return jnp.dot(a, b, preferred_element_type=F32)


def iota(shape, dim):
    return lax.broadcasted_iota(jnp.int32, shape, dim)


def half_turn(x):
    return jnp.concatenate([x[4:], x[:4]], axis=0)


def norm_rows(values, gain):
    scale = lax.rsqrt(jnp.mean(values * values, axis=-1, keepdims=True) + 1e-06)
    return values * scale * gain


def kernel(
    n, t,
    q_ref, k_ref, v_ref, bias_ref, ow_ref, mix_gain_ref, x_ref, ffn_gain_ref, ids_ref, score_ref, gw_ref, uw_ref, dw_ref,
    mixed_ref, moe_ref,
    gate, up, down, ow, kv, qm, acc, carry, out_buf, in_buf, back, ret, xb, total, marks, proj, proj_in,
    loc_sem, w_send, w_recv, f_send, f_recv, kv_send, kv_recv, d_send, d_recv, r_send, r_recv, p_send, p_recv,
):
    me, col = lax.axis_index("ep"), lax.axis_index("tp")
    span, width = q_ref.shape
    tokens, model = x_ref.shape
    heads = bias_ref.shape[0]
    pairs = heads // 2
    wide = model + model // 2
    right, left = lax.rem(col + 1, t), lax.rem(col + t - 1, t)
    far = lax.rem(col + 2, t)
    core = lax.rem(me, 2)
    partner = me + 1 - 2 * core
    chips = n // 2
    plus_steps, minus_steps = chips // 2, (chips - 1) // 2

    barrier = pltpu.get_barrier_semaphore()

    def greet(d, _):
        pl.semaphore_signal(barrier, inc=1, device_id={"ep": lax.rem(me + d, n)}, device_id_type=MESH)
        return 0

    lax.fori_loop(1, n, greet, 0)
    for d in range(1, t):
        pl.semaphore_signal(barrier, inc=1, device_id={"tp": lax.rem(col + d, t)}, device_id_type=MESH)

    local = [
        pltpu.make_async_copy(k_ref, kv.at[me, pl.ds(0, span)], loc_sem.at[0]),
        pltpu.make_async_copy(v_ref, kv.at[me, pl.ds(span, span)], loc_sem.at[1]),
        pltpu.make_async_copy(gw_ref.at[0], gate.at[col], loc_sem.at[2]),
        pltpu.make_async_copy(uw_ref.at[0], up.at[col], loc_sem.at[3]),
        pltpu.make_async_copy(dw_ref.at[0], down.at[col], loc_sem.at[4]),
        pltpu.make_async_copy(ow_ref, ow, loc_sem.at[5]),
    ]
    for c in local:
        c.start()
    kv[me, pl.ds(2 * span, ROWS), :] = jnp.zeros((ROWS, width), BF16)
    kv[me, pl.ds(2 * span, ROWS), 0:span] = bias_ref[...]

    normed = norm_rows(x_ref[...].astype(F32), ffn_gain_ref[...]).astype(BF16)
    first, second = ids_ref[0:1, :], ids_ref[1:2, :]
    expert = iota((n, tokens), 0)
    named0, named1 = expert == first, expert == second
    named = jnp.where(named0 | named1, 1.0, 0.0)
    before = jnp.where(iota((tokens, tokens), 0) < iota((tokens, tokens), 1), 1.0, 0.0).astype(BF16)
    place = dot(named.astype(BF16), before)
    place = jnp.where(named > 0.5, place, 127.0)
    scores = score_ref[...]
    weights = scores / jnp.sum(scores, axis=0, keepdims=True)
    weight = jnp.where(named0, weights[0:1, :], 0.0) + jnp.where(named1, weights[1:2, :], 0.0)
    high = weight.astype(BF16)
    low = (weight - high.astype(F32)).astype(BF16)
    slots = n * ROWS
    spread = jnp.where(iota((slots, n), 0) // ROWS == iota((slots, n), 1), 1.0, 0.0).astype(BF16)
    place = dot(spread, place.astype(BF16))
    high, low = dot(spread, high), dot(spread, low)
    row = lax.rem(iota((slots, tokens), 0), ROWS)
    rowf = row.astype(F32)
    main = jnp.where(place == rowf, 1.0, 0.0)
    upper = jnp.where((row < 4) & (place == rowf + 8.0), 1.0, 0.0)
    lower = jnp.where((row >= 4) & (place == rowf + 4.0), 1.0, 0.0)
    for i, m in enumerate((main, upper, lower)):
        marks[i, 0] = (m * high).T.astype(BF16)
        marks[i, 1] = (m * low).T.astype(BF16)
    half = model // 2
    out_buf[:, 0:model] = dot(main.astype(BF16), normed).astype(BF16)
    out_buf[:, model:wide] = (
        dot(upper.astype(BF16), normed[:, 0:half]) + dot(lower.astype(BF16), normed[:, half:model])
    ).astype(BF16)

    pl.semaphore_wait(barrier, n - 1 + t - 1)

    def rows_of(ref, slot, part):
        size = ref.shape[1] // 2
        return ref.at[slot, pl.ds(part * size, size)]

    weight_set = ((gw_ref, gate), (uw_ref, up), (dw_ref, down))

    def direct(w, way, part):
        src, dst = weight_set[w]
        return pltpu.make_async_remote_copy(
            src_ref=rows_of(src, 0, part), dst_ref=rows_of(dst, col, part),
            send_sem=w_send.at[way, w, part], recv_sem=w_recv.at[way, w, part],
            device_id={"tp": right if way == 0 else left}, device_id_type=MESH,
        )

    def arrived(w, way, part):
        src, dst = weight_set[w]
        return pltpu.make_async_remote_copy(
            src_ref=rows_of(src, 0, part), dst_ref=rows_of(dst, left if way == 0 else right, part),
            send_sem=w_send.at[way, w, part], recv_sem=w_recv.at[way, w, part],
            device_id={"tp": right if way == 0 else left}, device_id_type=MESH,
        )

    def forward(w, way):
        dst = weight_set[w][1]
        held = rows_of(dst, left if way == 0 else right, way)
        return pltpu.make_async_remote_copy(
            src_ref=held, dst_ref=held, send_sem=f_send.at[way, w], recv_sem=f_recv.at[way, w],
            device_id={"tp": right if way == 0 else left}, device_id_type=MESH,
        )

    def forwarded(w, way):
        dst = weight_set[w][1]
        held = rows_of(dst, far, way)
        return pltpu.make_async_remote_copy(
            src_ref=held, dst_ref=held, send_sem=f_send.at[way, w], recv_sem=f_recv.at[way, w],
            device_id={"tp": right if way == 0 else left}, device_id_type=MESH,
        )

    for part in range(2):
        for w in range(3):
            for way in range(2):
                direct(w, way, part if way == 0 else 1 - part).start()

    def kv_copy(slot, way):
        peer = (lax.rem(me + 2, n), lax.rem(me + n - 2, n), partner)[way]
        return pltpu.make_async_remote_copy(
            src_ref=kv.at[slot], dst_ref=kv.at[slot], send_sem=kv_send.at[way, slot], recv_sem=kv_recv.at[slot],
            device_id={"ep": peer}, device_id_type=MESH,
        )

    local[0].wait()
    local[1].wait()
    kv_copy(me, 0).start()
    if minus_steps > 0:
        kv_copy(me, 1).start()
    kv_copy(me, 2).start()

    def strip(ref, index):
        return ref.at[pl.ds(pl.multiple_of(index * ROWS, ROWS), ROWS)]

    def dispatch(peer):
        return pltpu.make_async_remote_copy(
            src_ref=strip(out_buf, peer), dst_ref=strip(in_buf, me), send_sem=d_send.at[peer], recv_sem=d_recv.at[me],
            device_id={"ep": peer}, device_id_type=MESH,
        )

    def dispatched(peer):
        return pltpu.make_async_remote_copy(
            src_ref=strip(out_buf, peer), dst_ref=strip(in_buf, peer), send_sem=d_send.at[peer], recv_sem=d_recv.at[peer],
            device_id={"ep": peer}, device_id_type=MESH,
        )

    def give_back(peer):
        return pltpu.make_async_remote_copy(
            src_ref=strip(back, peer), dst_ref=strip(ret, me), send_sem=r_send.at[peer], recv_sem=r_recv.at[me],
            device_id={"ep": peer}, device_id_type=MESH,
        )

    def given_back(peer):
        return pltpu.make_async_remote_copy(
            src_ref=strip(back, peer), dst_ref=strip(ret, peer), send_sem=r_send.at[peer], recv_sem=r_recv.at[peer],
            device_id={"ep": peer}, device_id_type=MESH,
        )

    def at_distance(i):
        step = (i + 1) // 2
        return lax.rem(me + jnp.where(lax.rem(i, 2) == 1, step, n - step), n)

    def each_peer(act):
        def body(i, _):
            act(at_distance(i))
            return 0

        lax.fori_loop(1, n, body, 0)

    each_peer(lambda peer: dispatch(peer).start())
    own_in = pltpu.make_async_copy(strip(out_buf, me), strip(in_buf, me), loc_sem.at[6])
    own_in.start()

    lane = iota((span, 2 * (width // heads)), 1)
    headed = width // heads
    for p in range(pairs):
        both = q_ref[:, 2 * headed * p : 2 * headed * (p + 1)].astype(F32) * headed ** (-0.5)
        qm[p, 0:span] = jnp.where(lane < headed, both, 0.0).astype(BF16)
        qm[p, span : 2 * span] = jnp.where(lane >= headed, both, 0.0).astype(BF16)
    acc[...] = jnp.zeros_like(acc)
    carry[...] = jnp.zeros_like(carry)

    for w in range(3):
        arrived(w, 0, 0).wait_recv()
        forward(w, 0).start()
        arrived(w, 1, 1).wait_recv()
        forward(w, 1).start()

    each_peer(lambda peer: dispatched(peer).wait_recv())
    own_in.wait()

    def kv_step(k):
        if k <= plus_steps:
            slot = lax.rem(me + n - 2 * k, n)
            kv_copy(slot, 0).wait_recv()
            if k < plus_steps:
                kv_copy(slot, 0).start()
            kv_copy(slot, 2).start()
        if k <= minus_steps:
            slot = lax.rem(me + 2 * k, n)
            kv_copy(slot, 1).wait_recv()
            if k < minus_steps:
                kv_copy(slot, 1).start()
            kv_copy(slot, 2).start()

    kv_step(1)

    xb[0:slots] = in_buf[:, 0:model]
    row8 = iota((ROWS, half), 0)

    def join(i, _):
        base = pl.multiple_of(i * 4 * ROWS, 4 * ROWS)
        four = in_buf[pl.ds(base, 4 * ROWS), model:wide].astype(F32)
        lefts, rights = [], []
        for j in range(2):
            even, odd = four[2 * ROWS * j : 2 * ROWS * j + ROWS], four[2 * ROWS * j + ROWS : 2 * ROWS * (j + 1)]
            lefts.append(jnp.where(row8 < 4, even, half_turn(odd)))
            rights.append(jnp.where(row8 < 4, half_turn(even), odd))
        to = pl.ds(pl.multiple_of(slots + i * 2 * ROWS, 2 * ROWS), 2 * ROWS)
        xb[to, 0:half] = jnp.concatenate(lefts, axis=0).astype(BF16)
        xb[to, half:model] = jnp.concatenate(rights, axis=0).astype(BF16)
        return 0

    lax.fori_loop(0, n // 4, join, 0)

    chunk = 512

    def serve(slot, number):
        rows = xb[...]
        g = dot(rows, gate[slot])
        u = dot(rows, up[slot])
        hidden = (g / (1.0 + jnp.exp(-g)) * u).astype(BF16)
        for c in range(model // chunk):
            at = slice(c * chunk, (c + 1) * chunk)
            term = dot(hidden, down[slot, :, at]).astype(BF16).astype(F32)
            if number == 0:
                total[:, at] = term
            else:
                total[:, at] += term

    for c in local[2:5]:
        c.wait()
    serve(col, 0)
    kv_step(2)
    for w in range(3):
        arrived(w, 0, 1).wait_recv()
    serve(left, 1)
    kv_step(3)
    for w in range(3):
        arrived(w, 1, 0).wait_recv()
    serve(right, 2)
    for k in range(4, 7):
        kv_step(k)
    for w in range(3):
        forwarded(w, 0).wait_recv()
        forwarded(w, 1).wait_recv()
    serve(far, 3)
    back[:, 0:model] = total[0:slots].astype(BF16)

    def part(i, _):
        at = pl.ds(pl.multiple_of(slots + i * ROWS, ROWS), ROWS)
        lefts, rights = total[at, 0:half], total[at, half:model]
        even = jnp.where(row8 < 4, lefts, half_turn(rights))
        odd = jnp.where(row8 < 4, half_turn(lefts), rights)
        to = pl.ds(pl.multiple_of(i * 2 * ROWS, 2 * ROWS), 2 * ROWS)
        back[to, model:wide] = jnp.concatenate([even, odd], axis=0).astype(BF16)
        return 0

    lax.fori_loop(0, n // 2, part, 0)
    each_peer(lambda peer: give_back(peer).start())
    own_back = pltpu.make_async_copy(strip(back, me), strip(ret, me), loc_sem.at[7])
    own_back.start()
    for k in range(7, plus_steps + 1):
        kv_step(k)

    def from_partner(i, _):
        kv_copy(2 * i + 1 - core, 2).wait_recv()
        return 0

    lax.fori_loop(0, chips, from_partner, 0)

    later = jnp.where(iota((2 * span, 2 * span), 0) % span > iota((2 * span, 2 * span), 1), 1.0, 0.0)
    later = jnp.where(iota((2 * span, 2 * span), 1) >= span, 1.0, later).astype(BF16)
    past = iota((2 * span, span), 1) < lax.rem(iota((2 * span, span), 0), span)

    def attend(block, masked):
        for p in range(pairs):
            lanes = slice(2 * headed * p, 2 * headed * (p + 1))
            z = lax.dot_general(
                qm[p], kv[block, 0:span, lanes], (((1,), (1,)), ((), ())), preferred_element_type=F32
            )
            bias = kv[block, 2 * span : 2 * span + ROWS, 0:span].astype(F32)
            z = jnp.concatenate(
                [z[0:span] + bias[2 * p : 2 * p + 1], z[span : 2 * span] + bias[2 * p + 1 : 2 * p + 2]], axis=0
            )
            soft = jnp.log(1.0 + jnp.exp(-jnp.abs(z)))
            rest = jnp.minimum(-z, 0.0) - soft
            if masked:
                rest = jnp.where(past, rest, 0.0)
            top = rest.astype(BF16)
            bottom = (rest - top.astype(F32)).astype(BF16)
            sums = dot(jnp.concatenate([top, bottom], axis=1), later)
            power = jnp.exp(jnp.minimum(z, 0.0) - soft + (sums[:, 0:span] + carry[p]))
            if masked:
                power = jnp.where(past, power, 0.0)
            carry[p] += sums[:, span : 2 * span]
            acc[p] += dot(power.astype(BF16), kv[block, span : 2 * span, lanes])

    attend(me, True)

    def earlier(i, _):
        attend(me - 1 - i, False)
        return 0

    lax.fori_loop(0, me, earlier, 0)

    attended = jnp.concatenate(
        [jnp.where(lane < headed, acc[p, 0:span], acc[p, span : 2 * span]) for p in range(pairs)], axis=1
    ).astype(BF16)
    local[5].wait()
    share = span // t
    proj[...] = dot(attended, ow[...]).astype(BF16)

    def shares(ref, index):
        return ref.at[pl.ds(pl.multiple_of(index * share, share), share)]

    def project(peer, slot):
        return pltpu.make_async_remote_copy(
            src_ref=shares(proj, peer), dst_ref=shares(proj_in, slot), send_sem=p_send.at[peer], recv_sem=p_recv.at[slot],
            device_id={"tp": peer}, device_id_type=MESH,
        )

    own_share = pltpu.make_async_copy(shares(proj, col), shares(proj_in, col), loc_sem.at[8])
    own_share.start()
    for d in range(1, t):
        project(lax.rem(col + d, t), col).start()
    own_share.wait()
    for d in range(1, t):
        peer = lax.rem(col + d, t)
        project(peer, peer).wait_recv()
    projected = proj_in[0:share].astype(F32)
    for i in range(1, t):
        projected = projected + proj_in[i * share : (i + 1) * share].astype(F32)
    mixed_ref[...] = norm_rows(projected, mix_gain_ref[...]).astype(BF16)

    each_peer(lambda peer: given_back(peer).wait_recv())
    own_back.wait()
    for c in range(2):
        at = slice(c * half, (c + 1) * half)
        tail = ret[:, model:wide]
        mix = dot(marks[0, 0], ret[:, at]) + dot(marks[0, 1], ret[:, at])
        mix = mix + dot(marks[1 + c, 0], tail) + dot(marks[1 + c, 1], tail)
        moe_ref[:, at] = mix.astype(BF16)

    for w in range(3):
        for way in range(2):
            forward(w, way).wait_send()
            for s in range(2):
                direct(w, way, s).wait_send()

    def left_here(peer):
        dispatch(peer).wait_send()
        give_back(peer).wait_send()

    each_peer(left_here)
    for k in range(plus_steps):
        kv_copy(lax.rem(me + n - 2 * k, n), 0).wait_send()
    for k in range(minus_steps):
        kv_copy(lax.rem(me + 2 * k, n), 1).wait_send()

    def to_partner(i, _):
        kv_copy(2 * i + core, 2).wait_send()
        return 0

    lax.fori_loop(0, chips, to_partner, 0)
    for d in range(1, t):
        project(lax.rem(col + d, t), col).wait_send()


def per_device(
    queries, keys, values, stop_bias, out_weight, mix_gain, moe_input, ffn_gain, expert_ids, expert_scores,
    gate_weight, up_weight, down_weight,
):
    n, t = lax.axis_size("ep"), lax.axis_size("tp")
    span, width = queries.shape
    heads = stop_bias.shape[1]
    tokens, model = moe_input.shape
    hidden = gate_weight.shape[2]
    slots, wide, pairs = n * ROWS, model + model // 2, heads // 2
    vmem, anywhere = pl.BlockSpec(memory_space=pltpu.VMEM), pl.BlockSpec(memory_space=pl.ANY)
    dma = pltpu.SemaphoreType.DMA
    return pl.pallas_call(
        functools.partial(kernel, n, t),
        out_shape=(
            jax.ShapeDtypeStruct((span // t, model), BF16),
            jax.ShapeDtypeStruct((tokens, model), BF16),
        ),
        in_specs=[
            vmem, anywhere, anywhere, vmem, anywhere, vmem, vmem, vmem, vmem, vmem, anywhere, anywhere, anywhere,
        ],
        out_specs=(vmem, vmem),
        scratch_shapes=[
            pltpu.VMEM((t, model, hidden), BF16),
            pltpu.VMEM((t, model, hidden), BF16),
            pltpu.VMEM((t, hidden, model), BF16),
            pltpu.VMEM(out_weight.shape, BF16),
            pltpu.VMEM((n, 2 * span + ROWS, width), BF16),
            pltpu.VMEM((pairs, 2 * span, 2 * width // heads), BF16),
            pltpu.VMEM((pairs, 2 * span, 2 * width // heads), F32),
            pltpu.VMEM((pairs, 2 * span, span), F32),
            pltpu.VMEM((slots, wide), BF16),
            pltpu.VMEM((slots, wide), BF16),
            pltpu.VMEM((slots, wide), BF16),
            pltpu.VMEM((slots, wide), BF16),
            pltpu.VMEM((slots + slots // 2, model), BF16),
            pltpu.VMEM((slots + slots // 2, model), F32),
            pltpu.VMEM((3, 2, tokens, slots), BF16),
            pltpu.VMEM((span, model), BF16),
            pltpu.VMEM((span, model), BF16),
            dma((9,)),
            dma((2, 3, 2)),
            dma((2, 3, 2)),
            dma((2, 3)),
            dma((2, 3)),
            dma((3, n)),
            dma((n,)),
            dma((n,)),
            dma((n,)),
            dma((n,)),
            dma((n,)),
            dma((t,)),
            dma((t,)),
        ],
        compiler_params=pltpu.CompilerParams(
            collective_id=0, has_side_effects=True, vmem_limit_bytes=60 * 1024 * 1024
        ),
    )(
        queries, keys, values, stop_bias.T, out_weight, mix_gain[None, :], moe_input, ffn_gain[None, :],
        expert_ids.T, expert_scores.T, gate_weight, up_weight, down_weight,
    )


def solution(mesh):
    placed = (
        P(GRP_EP, "tp"), P(GRP_EP, "tp"), P(GRP_EP, "tp"), P(GRP_EP, "tp"), P("tp", None), P(), P(GRP_EP_TP, None), P(),
        P(GRP_EP_TP, None), P(GRP_EP_TP, None), P("ep", None, "tp"), P("ep", None, "tp"), P("ep", "tp", None),
    )
    return jax.shard_map(
        per_device,
        mesh=mesh,
        in_specs=placed,
        out_specs=(P(GRP_EP_TP, None), P(GRP_EP_TP, None)),
        check_vma=False,
    )
```

```python
import contextlib
import functools

import jax
import jax.numpy as jnp
from jax import lax
from jax.experimental import pallas as pl
from jax.experimental.pallas import tpu as pltpu
from jax.sharding import PartitionSpec as P

MESH = pl.DeviceIdType.MESH
BF16 = jnp.bfloat16
F32 = jnp.float32
GRP_EP = ("grp", "ep")
GRP_EP_TP = ("grp", "ep", "tp")
ROWS = 8


def scope(name):
    return contextlib.nullcontext()


def dot(a, b):
    return jnp.dot(a, b, preferred_element_type=F32)


def iota(shape, dim):
    return lax.broadcasted_iota(jnp.int32, shape, dim)


def half_turn(x):
    return jnp.concatenate([x[4:], x[:4]], axis=0)


def norm_rows(values, gain):
    scale = lax.rsqrt(jnp.mean(values * values, axis=-1, keepdims=True) + 1e-06)
    return values * scale * gain


def kernel(
    n, t,
    q_ref, k_ref, v_ref, bias_ref, ow_ref, mix_gain_ref, x_ref, ffn_gain_ref, ids_ref, score_ref, gw_ref, uw_ref, dw_ref,
    mixed_ref, moe_ref,
    gate, up, down, ow, q_out, q_in, kv_out, kv_in, a_out, a_in, qm, acc, carry,
    out_buf, in_buf, back, ret, xb, total, marks, proj, proj_in,
    loc_sem, w_send, w_recv, f_send, f_recv, q_send, q_recv, kv_send, kv_recv, c_send, a_send, a_recv,
    d_send, d_recv, r_send, r_recv, p_send, p_recv,
):
    me, col = lax.axis_index("ep"), lax.axis_index("tp")
    span, width = q_ref.shape
    tokens, model = x_ref.shape
    heads = bias_ref.shape[0]
    headed = width // heads
    pairs = heads // 2
    wide = model + model // 2
    right, left = lax.rem(col + 1, t), lax.rem(col + t - 1, t)
    far = lax.rem(col + 2, t)
    core = lax.rem(me, 2)
    partner = me + 1 - 2 * core
    crew = n // heads
    head, member = me // crew, lax.rem(me, crew)

    barrier = pltpu.get_barrier_semaphore()

    def greet(d, _):
        pl.semaphore_signal(barrier, inc=1, device_id={"ep": lax.rem(me + d, n)}, device_id_type=MESH)
        return 0

    lax.fori_loop(1, n, greet, 0)
    for d in range(1, t):
        pl.semaphore_signal(barrier, inc=1, device_id={"tp": lax.rem(col + d, t)}, device_id_type=MESH)

    local = [
        pltpu.make_async_copy(gw_ref.at[0], gate.at[col], loc_sem.at[2]),
        pltpu.make_async_copy(uw_ref.at[0], up.at[col], loc_sem.at[3]),
        pltpu.make_async_copy(dw_ref.at[0], down.at[col], loc_sem.at[4]),
        pltpu.make_async_copy(ow_ref, ow, loc_sem.at[5]),
    ]
    for c in local:
        c.start()

    side = span // 2
    lane = iota((span, 2 * headed), 1)
    lane_side = iota((side, 2 * headed), 1)
    swap = functools.partial(pltpu.roll, shift=headed, axis=1)
    with scope("pack"):
        for p in range(pairs):
            lanes = slice(2 * headed * p, 2 * headed * (p + 1))
            q = q_ref[:, lanes].astype(F32) * headed ** (-0.5)
            k, v = k_ref[:, lanes].astype(F32), v_ref[:, lanes].astype(F32)
            q_out[2 * p] = jnp.where(lane_side < headed, q[0:side], swap(q[side:span])).astype(BF16)
            q_out[2 * p + 1] = jnp.where(lane_side < headed, swap(q[0:side]), q[side:span]).astype(BF16)
            kv_out[2 * p, 0:span] = jnp.where(lane < headed, k, swap(v)).astype(BF16)
            kv_out[2 * p + 1, 0:span] = jnp.where(lane < headed, swap(k), v).astype(BF16)
        odds = bias_ref[...].astype(F32)
        for h in range(heads):
            kv_out[h, span : span + ROWS] = jnp.broadcast_to(odds[h : h + 1], (ROWS, span)).astype(BF16)

    with scope("plan"):
        normed = norm_rows(x_ref[...].astype(F32), ffn_gain_ref[...]).astype(BF16)
        first, second = ids_ref[0:1, :], ids_ref[1:2, :]
        expert = iota((n, tokens), 0)
        named0, named1 = expert == first, expert == second
        named = jnp.where(named0 | named1, 1.0, 0.0)
        before = jnp.where(iota((tokens, tokens), 0) < iota((tokens, tokens), 1), 1.0, 0.0).astype(BF16)
        place = dot(named.astype(BF16), before)
        place = jnp.where(named > 0.5, place, 127.0)
        scores = score_ref[...]
        weights = scores / jnp.sum(scores, axis=0, keepdims=True)
        weight = jnp.where(named0, weights[0:1, :], 0.0) + jnp.where(named1, weights[1:2, :], 0.0)
        high = weight.astype(BF16)
        low = (weight - high.astype(F32)).astype(BF16)
        slots = n * ROWS
        spread = jnp.where(iota((slots, n), 0) // ROWS == iota((slots, n), 1), 1.0, 0.0).astype(BF16)
        place = dot(spread, place.astype(BF16))
        high, low = dot(spread, high), dot(spread, low)
        row = lax.rem(iota((slots, tokens), 0), ROWS)
        rowf = row.astype(F32)
        main = jnp.where(place == rowf, 1.0, 0.0)
        upper = jnp.where((row < 4) & (place == rowf + 8.0), 1.0, 0.0)
        lower = jnp.where((row >= 4) & (place == rowf + 4.0), 1.0, 0.0)
        for i, m in enumerate((main, upper, lower)):
            marks[i, 0] = (m * high).T.astype(BF16)
            marks[i, 1] = (m * low).T.astype(BF16)
        half = model // 2
        out_buf[:, 0:model] = dot(main.astype(BF16), normed).astype(BF16)
        out_buf[:, model:wide] = (
            dot(upper.astype(BF16), normed[:, 0:half]) + dot(lower.astype(BF16), normed[:, half:model])
        ).astype(BF16)

    with scope("barrier"):
        pl.semaphore_wait(barrier, n - 1 + t - 1)

    def rows_of(ref, slot, part):
        size = ref.shape[1] // 2
        return ref.at[slot, pl.ds(part * size, size)]

    weight_set = ((gw_ref, gate), (uw_ref, up), (dw_ref, down))

    def side_copy(src, dst, sends, recvs, way):
        return pltpu.make_async_remote_copy(
            src_ref=src, dst_ref=dst, send_sem=sends, recv_sem=recvs,
            device_id={"tp": right if way == 0 else left}, device_id_type=MESH,
        )

    def direct(w, way, part, slot=col):
        src, dst = weight_set[w]
        return side_copy(
            rows_of(src, 0, part), rows_of(dst, slot, part), w_send.at[way, w, part], w_recv.at[way, w, part], way
        )

    def arrived(w, way, part):
        return direct(w, way, part, left if way == 0 else right)

    def forward(w, way, slot=None):
        held = rows_of(weight_set[w][1], (left if way == 0 else right) if slot is None else slot, way)
        return side_copy(held, held, f_send.at[way, w], f_recv.at[way, w], way)

    def forwarded(w, way):
        return forward(w, way, far)

    for part in range(2):
        for w in range(3):
            for way in range(2):
                direct(w, way, part if way == 0 else 1 - part).start()

    def along(src, dst, sends, recvs, peer):
        return pltpu.make_async_remote_copy(
            src_ref=src, dst_ref=dst, send_sem=sends, recv_sem=recvs, device_id={"ep": peer}, device_id_type=MESH
        )

    def send_q(h):
        return along(q_out.at[h], q_in.at[head], q_send.at[h], q_recv.at[head], crew * h + member)

    def got_q(j):
        return along(q_out.at[j], q_in.at[j], q_send.at[j], q_recv.at[j], crew * j + member)

    def send_kv(h, c):
        return along(kv_out.at[h], kv_in.at[me], kv_send.at[h, c], kv_recv.at[me], crew * h + 2 * c + core)

    def got_kv(source):
        return along(kv_out.at[0], kv_in.at[source], kv_send.at[0, 0], kv_recv.at[source], partner)

    def share_kv(source):
        return along(kv_in.at[source], kv_in.at[source], c_send.at[source], kv_recv.at[source], partner)

    chip, chips = member // 2, crew // 2
    order = sorted(range(1, heads), key=lambda d: (min(d, heads - d), d))
    own_q = pltpu.make_async_copy(q_out.at[head], q_in.at[head], loc_sem.at[0])
    own_kv = pltpu.make_async_copy(kv_out.at[head], kv_in.at[me], loc_sem.at[1])
    own_q.start()
    own_kv.start()
    for d in order:
        h = lax.rem(head + d, heads)
        for c in range(chips):
            send_kv(h, c).start()
        send_q(h).start()
    for c in range(1, chips):
        send_kv(head, lax.rem(chip + c, chips)).start()

    def strip(ref, index):
        return ref.at[pl.ds(pl.multiple_of(index * ROWS, ROWS), ROWS)]

    def dispatch(peer):
        return along(strip(out_buf, peer), strip(in_buf, me), d_send.at[peer], d_recv.at[me], peer)

    def dispatched(peer):
        return along(strip(out_buf, peer), strip(in_buf, peer), d_send.at[peer], d_recv.at[peer], peer)

    def give_back(peer):
        return along(strip(back, peer), strip(ret, me), r_send.at[peer], r_recv.at[me], peer)

    def given_back(peer):
        return along(strip(back, peer), strip(ret, peer), r_send.at[peer], r_recv.at[peer], peer)

    def each_peer(act):
        def body(i, _):
            step = (i + 1) // 2
            act(lax.rem(me + jnp.where(lax.rem(i, 2) == 1, step, n - step), n))
            return 0

        lax.fori_loop(1, n, body, 0)

    with scope("issue"):
        each_peer(lambda peer: dispatch(peer).start())
        own_in = pltpu.make_async_copy(strip(out_buf, me), strip(in_buf, me), loc_sem.at[6])
        own_in.start()

    acc[...] = jnp.zeros_like(acc)
    carry[...] = jnp.zeros_like(carry)

    with scope("kvwait"):
        own_kv.wait()
        share_kv(me).start()

        def pass_on(i, _):
            source = lax.rem(me + 2 * i, n)
            got_kv(source).wait_recv()
            share_kv(source).start()
            return 0

        lax.fori_loop(1, n // 2, pass_on, 0)
        own_q.wait()
        for d in order:
            got_q(lax.rem(head + d, heads)).wait_recv()

        def from_partner(i, _):
            got_kv(2 * i + 1 - core).wait_recv()
            return 0

        lax.fori_loop(0, n // 2, from_partner, 0)

    for p in range(pairs):
        for s in range(2):
            q = q_in[heads - 1 - 2 * p - s].astype(F32)
            qm[p, span * s : span * s + side] = jnp.where(lane_side < headed, q, 0.0).astype(BF16)
            qm[p, span * s + side : span * (s + 1)] = jnp.where(lane_side < headed, swap(q), 0.0).astype(BF16)
    later = jnp.where(iota((2 * span, 2 * span), 0) % span > iota((2 * span, 2 * span), 1), 1.0, 0.0)
    later = jnp.where(iota((2 * span, 2 * span), 1) >= span, 1.0, later).astype(BF16)
    row = iota((2 * span, span), 0)
    ahead = iota((2 * span, span), 1) - jnp.where(row < span, row, row - span - crew * span)

    def last_block(p):
        return crew * (heads - 1 - 2 * p) + member

    def attend(block, p, masked):
        z = lax.dot_general(qm[p], kv_in[block, 0:span], (((1,), (1,)), ((), ())), preferred_element_type=F32)
        z = z + kv_in[block, span : span + ROWS].astype(F32)[0:1]
        soft = jnp.log(1.0 + jnp.exp(-jnp.abs(z)))
        rest = jnp.minimum(-z, 0.0) - soft
        if masked:
            past = ahead < (last_block(p) - block) * span
            rest = jnp.where(past, rest, 0.0)
        top = rest.astype(BF16)
        bottom = (rest - top.astype(F32)).astype(BF16)
        sums = dot(jnp.concatenate([top, bottom], axis=1), later)
        power = jnp.exp(jnp.minimum(z, 0.0) - soft + (sums[:, 0:span] + carry[p]))
        if masked:
            power = jnp.where(past, power, 0.0)
        carry[p] += sums[:, span : 2 * span]
        acc[p] += dot(power.astype(BF16), kv_in[block, 0:span])

    def segment(s):
        def body(i, _):
            block = last_block(s) - i
            for p in range(s):
                attend(block, p, False)
            attend(block, s, True)
            return 0

        lax.fori_loop(0, 2 * crew if s < pairs - 1 else crew + member + 1, body, 0)

    for s in range(pairs):
        with scope(f"attend{s}"):
            segment(s)
        if s == max(pairs - 3, 0):
            with scope("wfwd"):
                for w in range(3):
                    for way in range(2):
                        arrived(w, way, way).wait_recv()
                        forward(w, way).start()

    def send_a(j):
        return along(a_out.at[j], a_in.at[head], a_send.at[j], a_recv.at[head], crew * j + member)

    def got_a(h):
        return along(a_out.at[h], a_in.at[h], a_send.at[h], a_recv.at[h], crew * h + member)

    with scope("asend"):
        for p in range(pairs):
            for s in range(2):
                a = acc[p, span * s : span * (s + 1)]
                a_out[heads - 1 - 2 * p - s] = jnp.where(lane_side < headed, swap(a[0:side]), a[side:span]).astype(BF16)
        own_a = pltpu.make_async_copy(a_out.at[head], a_in.at[head], loc_sem.at[9])
        own_a.start()
        for d in order:
            send_a(lax.rem(head + d, heads)).start()

    with scope("dwait"):
        each_peer(lambda peer: dispatched(peer).wait_recv())
        own_in.wait()

    xb[0:slots] = in_buf[:, 0:model]
    row8 = iota((ROWS, half), 0)

    def join(i, _):
        base = pl.multiple_of(i * 4 * ROWS, 4 * ROWS)
        four = in_buf[pl.ds(base, 4 * ROWS), model:wide].astype(F32)
        lefts, rights = [], []
        for j in range(2):
            even, odd = four[2 * ROWS * j : 2 * ROWS * j + ROWS], four[2 * ROWS * j + ROWS : 2 * ROWS * (j + 1)]
            lefts.append(jnp.where(row8 < 4, even, half_turn(odd)))
            rights.append(jnp.where(row8 < 4, half_turn(even), odd))
        to = pl.ds(pl.multiple_of(slots + i * 2 * ROWS, 2 * ROWS), 2 * ROWS)
        xb[to, 0:half] = jnp.concatenate(lefts, axis=0).astype(BF16)
        xb[to, half:model] = jnp.concatenate(rights, axis=0).astype(BF16)
        return 0

    lax.fori_loop(0, n // 4, join, 0)

    chunk = 512

    def serve(slot, number):
        rows = xb[...]
        g = dot(rows, gate[slot])
        u = dot(rows, up[slot])
        hidden = (g / (1.0 + jnp.exp(-g)) * u).astype(BF16)
        for c in range(model // chunk):
            at = slice(c * chunk, (c + 1) * chunk)
            term = dot(hidden, down[slot, :, at]).astype(BF16).astype(F32)
            if number == 0:
                total[:, at] = term
            else:
                total[:, at] += term

    with scope("serve3"):
        for c in local[0:3]:
            c.wait()
        serve(col, 0)
        for w in range(3):
            arrived(w, 0, 1).wait_recv()
        serve(left, 1)
        for w in range(3):
            arrived(w, 1, 0).wait_recv()
        serve(right, 2)
    with scope("farwait"):
        for w in range(3):
            forwarded(w, 0).wait_recv()
            forwarded(w, 1).wait_recv()
    with scope("serve1"):
        serve(far, 3)
        back[:, 0:model] = total[0:slots].astype(BF16)

        def part(i, _):
            at = pl.ds(pl.multiple_of(slots + i * ROWS, ROWS), ROWS)
            lefts, rights = total[at, 0:half], total[at, half:model]
            even = jnp.where(row8 < 4, lefts, half_turn(rights))
            odd = jnp.where(row8 < 4, half_turn(lefts), rights)
            to = pl.ds(pl.multiple_of(i * 2 * ROWS, 2 * ROWS), 2 * ROWS)
            back[to, model:wide] = jnp.concatenate([even, odd], axis=0).astype(BF16)
            return 0

        lax.fori_loop(0, n // 2, part, 0)
    each_peer(lambda peer: give_back(peer).start())
    own_back = pltpu.make_async_copy(strip(back, me), strip(ret, me), loc_sem.at[7])
    own_back.start()

    with scope("await"):
        own_a.wait()
        for d in order:
            got_a(lax.rem(head + d, heads)).wait_recv()
        local[3].wait()
    columns = []
    for p in range(pairs):
        a, b = a_in[2 * p].astype(F32), a_in[2 * p + 1].astype(F32)
        columns.append(
            jnp.concatenate(
                [jnp.where(lane_side < headed, a, swap(b)), jnp.where(lane_side < headed, swap(a), b)], axis=0
            )
        )
    attended = jnp.concatenate(columns, axis=1).astype(BF16)
    share = span // t
    proj[...] = dot(attended, ow[...]).astype(BF16)

    def shares(ref, index):
        return ref.at[pl.ds(pl.multiple_of(index * share, share), share)]

    def project(peer, slot):
        return pltpu.make_async_remote_copy(
            src_ref=shares(proj, peer), dst_ref=shares(proj_in, slot), send_sem=p_send.at[peer], recv_sem=p_recv.at[slot],
            device_id={"tp": peer}, device_id_type=MESH,
        )

    own_share = pltpu.make_async_copy(shares(proj, col), shares(proj_in, col), loc_sem.at[8])
    own_share.start()
    for d in range(1, t):
        project(lax.rem(col + d, t), col).start()
    own_share.wait()
    with scope("pwait"):
        for d in range(1, t):
            peer = lax.rem(col + d, t)
            project(peer, peer).wait_recv()
    projected = proj_in[0:share].astype(F32)
    for i in range(1, t):
        projected = projected + proj_in[i * share : (i + 1) * share].astype(F32)
    mixed_ref[...] = norm_rows(projected, mix_gain_ref[...]).astype(BF16)

    with scope("retwait"):
        each_peer(lambda peer: given_back(peer).wait_recv())
        own_back.wait()
    with scope("combine"):
        for c in range(2):
            at = slice(c * half, (c + 1) * half)
            tail = ret[:, model:wide]
            mix = dot(marks[0, 0], ret[:, at]) + dot(marks[0, 1], ret[:, at])
            mix = mix + dot(marks[1 + c, 0], tail) + dot(marks[1 + c, 1], tail)
            moe_ref[:, at] = mix.astype(BF16)

    for w in range(3):
        for way in range(2):
            forward(w, way).wait_send()
            for s in range(2):
                direct(w, way, s).wait_send()
    for d in order:
        h = lax.rem(head + d, heads)
        send_q(h).wait_send()
        send_a(h).wait_send()
        for c in range(chips):
            send_kv(h, c).wait_send()
    for c in range(1, chips):
        send_kv(head, lax.rem(chip + c, chips)).wait_send()

    def left_here(peer):
        dispatch(peer).wait_send()
        give_back(peer).wait_send()

    each_peer(left_here)

    def to_partner(i, _):
        share_kv(2 * i + core).wait_send()
        return 0

    lax.fori_loop(0, n // 2, to_partner, 0)
    for d in range(1, t):
        project(lax.rem(col + d, t), col).wait_send()


def per_device(
    queries, keys, values, stop_bias, out_weight, mix_gain, moe_input, ffn_gain, expert_ids, expert_scores,
    gate_weight, up_weight, down_weight,
):
    n, t = lax.axis_size("ep"), lax.axis_size("tp")
    span, width = queries.shape
    heads = stop_bias.shape[1]
    tokens, model = moe_input.shape
    hidden = gate_weight.shape[2]
    slots, wide, pairs, lanes = n * ROWS, model + model // 2, heads // 2, 2 * width // heads
    vmem, anywhere = pl.BlockSpec(memory_space=pltpu.VMEM), pl.BlockSpec(memory_space=pl.ANY)
    dma = pltpu.SemaphoreType.DMA
    return pl.pallas_call(
        functools.partial(kernel, n, t),
        out_shape=(
            jax.ShapeDtypeStruct((span // t, model), BF16),
            jax.ShapeDtypeStruct((tokens, model), BF16),
        ),
        in_specs=[
            vmem, vmem, vmem, vmem, anywhere, vmem, vmem, vmem, vmem, vmem, anywhere, anywhere, anywhere,
        ],
        out_specs=(vmem, vmem),
        scratch_shapes=[
            pltpu.VMEM((t, model, hidden), BF16),
            pltpu.VMEM((t, model, hidden), BF16),
            pltpu.VMEM((t, hidden, model), BF16),
            pltpu.VMEM(out_weight.shape, BF16),
            pltpu.VMEM((heads, span // 2, lanes), BF16),
            pltpu.VMEM((heads, span // 2, lanes), BF16),
            pltpu.VMEM((heads, span + ROWS, lanes), BF16),
            pltpu.VMEM((n, span + ROWS, lanes), BF16),
            pltpu.VMEM((heads, span // 2, lanes), BF16),
            pltpu.VMEM((heads, span // 2, lanes), BF16),
            pltpu.VMEM((pairs, 2 * span, lanes), BF16),
            pltpu.VMEM((pairs, 2 * span, lanes), F32),
            pltpu.VMEM((pairs, 2 * span, span), F32),
            pltpu.VMEM((slots, wide), BF16),
            pltpu.VMEM((slots, wide), BF16),
            pltpu.VMEM((slots, wide), BF16),
            pltpu.VMEM((slots, wide), BF16),
            pltpu.VMEM((slots + slots // 2, model), BF16),
            pltpu.VMEM((slots + slots // 2, model), F32),
            pltpu.VMEM((3, 2, tokens, slots), BF16),
            pltpu.VMEM((span, model), BF16),
            pltpu.VMEM((span, model), BF16),
            dma((10,)),
            dma((2, 3, 2)),
            dma((2, 3, 2)),
            dma((2, 3)),
            dma((2, 3)),
            dma((heads,)),
            dma((heads,)),
            dma((heads, n // heads // 2)),
            dma((n,)),
            dma((n,)),
            dma((heads,)),
            dma((heads,)),
            dma((n,)),
            dma((n,)),
            dma((n,)),
            dma((n,)),
            dma((t,)),
            dma((t,)),
        ],
        compiler_params=pltpu.CompilerParams(
            collective_id=0, has_side_effects=True, vmem_limit_bytes=60 * 1024 * 1024
        ),
    )(
        queries, keys, values, stop_bias.T, out_weight, mix_gain[None, :], moe_input, ffn_gain[None, :],
        expert_ids.T, expert_scores.T, gate_weight, up_weight, down_weight,
    )


def solution(mesh):
    placed = (
        P(GRP_EP, "tp"), P(GRP_EP, "tp"), P(GRP_EP, "tp"), P(GRP_EP, "tp"), P("tp", None), P(), P(GRP_EP_TP, None), P(),
        P(GRP_EP_TP, None), P(GRP_EP_TP, None), P("ep", None, "tp"), P("ep", None, "tp"), P("ep", "tp", None),
    )
    return jax.shard_map(
        per_device,
        mesh=mesh,
        in_specs=placed,
        out_specs=(P(GRP_EP_TP, None), P(GRP_EP_TP, None)),
        check_vma=False,
    )
```
